32 devices in a mesh: rep: 4 (over z), fs: 4 (over y, x), tp: 2 (over core).
Axes of the slice: x: 2, y: 2, z: 4, core: 2. Of those that a mesh axis runs over, the one named last changes fastest.
Arguments:
- residual: bfloat16 [16, 256, 2048], P(('rep', 'fs'), None, 'tp'), may hold values from -6 to 6
- queries: bfloat16 [16, 256, 2048], P(('rep', 'fs'), None, 'tp'), may hold values from -6 to 6
- key_matrix: bfloat16 [16, 256, 2048], P(('rep', 'fs'), None, 'tp'), may hold values from -6 to 6
- value_matrix: bfloat16 [16, 256, 2048], P(('rep', 'fs'), None, 'tp'), may hold values from -6 to 6
- decay_logodds: float32 [16, 256, 2048], P(('rep', 'fs'), None, 'tp'), may hold values from -3.4 to 8.9, as said below
- decay_surge: float32 [16, 256, 8], P(('rep', 'fs'), None, 'tp'), may hold values from -2.1 to 0, as said below
- head_norm_gain: float32 [256], replicated, may hold values from 0.1 to 1.9
- output_matrix: float32 [2048, 2048], P('fs', 'tp'), may hold values from -0.125 to 0.125
- output_column_scale: float32 [2048], P('tp'), may hold values from 0.5 to 2
- premix_norm_gain: float32 [2048], replicated, may hold values from 0.1 to 1.9
- gate_matrix: float32 [2048, 2816], P('fs', 'tp'), may hold values from -0.125 to 0.125
- gate_column_scale: float32 [2816], P('tp'), may hold values from 0.5 to 2
- up_matrix: float32 [2048, 2816], P('fs', 'tp'), may hold values from -0.125 to 0.125
- up_column_scale: float32 [2816], P('tp'), may hold values from 0.5 to 2
- down_matrix: float32 [2048, 2816], P('fs', 'tp'), may hold values from -0.109375 to 0.109375
- down_column_scale: float32 [2048], P('tp'), may hold values from 0.5 to 2
Outputs:
- layer_out: bfloat16 [16, 256, 2048], P(('rep', 'fs'), None, 'tp')
The draws below stay inside these ranges and needn't reach their ends.
Inputs may be any that keep to these rules, and one draw needn't show every extreme that they name: `decay_logodds`: log-odds of a key channel's decay. `decay_surge`: non-positive log-factors of a head's state.
All inputs are finite; a program needn't handle non-finite values.
Results may differ from the reference program's by a relative error of at most 0.018.
Values may be sent and summed in bfloat16 or wider, within the bound.
A program may use at most 128 MiB of HBM per device.

```python
import math
import jax
import jax.numpy as jnp
from jax import lax

D = 2048
HEAD_NUMBER = 8
HEAD_V = 256
FF = 2816
BLOCK = 64
SEQUENCE_LENGTH = 256
KEY_DIM = 2048
VALUE_DIM = 2048
BATCH_SIZE = 16
N_TP = 2


def draw_decay_logodds(key, part):
    residual_flows = jax.random.split(jax.random.fold_in(key, 11), 5)
    slow_share = 0.5
    jitter = jnp.clip(0.7 * jax.random.normal(residual_flows[4], (BATCH_SIZE, SEQUENCE_LENGTH, KEY_DIM), jnp.float32), -2.8, 2.8)
    slow_mask = jax.random.uniform(residual_flows[0], (KEY_DIM,), jnp.float32) < slow_share
    slow_base = jax.random.uniform(residual_flows[1], (KEY_DIM,), jnp.float32, 3.5, 5.5)
    fast_base = jax.random.uniform(residual_flows[2], (KEY_DIM,), jnp.float32, 0.0, 1.2)
    offset = jax.random.uniform(residual_flows[3], (BATCH_SIZE, 1, 1), jnp.float32, -0.6, 0.6)
    return jnp.where(slow_mask, slow_base, fast_base) + offset + jitter


def draw_decay_surge(key, part):
    residual_flows = jax.random.split(jax.random.fold_in(key, 23), 2)
    surge_position = jax.random.randint(residual_flows[0], (BATCH_SIZE, 3, HEAD_NUMBER), 0, SEQUENCE_LENGTH)
    strength = jnp.log(jax.random.uniform(residual_flows[1], (BATCH_SIZE, 3, HEAD_NUMBER), jnp.float32, 0.5, 0.8))
    match_scores = jnp.arange(SEQUENCE_LENGTH)[None, :, None, None] == surge_position[:, None, :, :]
    return jnp.sum(jnp.where(match_scores, strength[:, None, :, :], 0.0), axis=2)


def block_levels(own_key, shape, cuts, low, top_value):
    def one(position, shards_of):
        draws = jax.random.uniform(jax.random.fold_in(jax.random.fold_in(own_key, 6), position), (shards_of,), jnp.float32, low / len(cuts), top_value / len(cuts))
        return jnp.repeat(jnp.exp(draws), shape[position] // shards_of).reshape((-1,) + (1,) * (len(shape) - position - 1))

    loudness = one(*cuts[0])
    for cut in cuts[1:]:
        loudness = loudness * one(*cut)
    return loudness


def gaussian(stream_key, dims, scale, bound, cuts=(), kind=jnp.bfloat16):
    values = jax.random.normal(stream_key, dims, jnp.float32) * scale
    if len(cuts) > 0:
        values = block_levels(stream_key, dims, cuts, -0.22, 0.18) * values
    return jnp.clip(values, min=-bound, max=bound).astype(kind)


def setup_inputs(seed: int = 0) -> dict:
    arg_keys = jax.random.split(jax.random.key(seed), 17)
    return {
        "residual": gaussian(arg_keys[0], (BATCH_SIZE, SEQUENCE_LENGTH, D), 1.0, 6.0, ((0, 16), (2, 2))),
        "queries": gaussian(arg_keys[1], (BATCH_SIZE, SEQUENCE_LENGTH, KEY_DIM), 1.0, 6.0, ((0, 16), (2, 2))),
        "key_matrix": gaussian(arg_keys[2], (BATCH_SIZE, SEQUENCE_LENGTH, KEY_DIM), 1.0, 6.0, ((0, 16), (2, 2))),
        "value_matrix": gaussian(arg_keys[3], (BATCH_SIZE, SEQUENCE_LENGTH, VALUE_DIM), 1.0, 6.0, ((0, 16), (2, 2))),
        "decay_logodds": draw_decay_logodds(jax.random.fold_in(arg_keys[16], 71), 0),
        "decay_surge": draw_decay_surge(jax.random.fold_in(arg_keys[16], 71), 0),
        "head_norm_gain": jnp.clip(1.0 + 0.18 * jax.random.normal(arg_keys[6], (HEAD_V,), jnp.float32), 0.1, 1.9),
        "output_matrix": gaussian(arg_keys[7], (D, VALUE_DIM), VALUE_DIM ** -0.5, 0.125, ((0, 4), (1, 2)), jnp.float32),
        "output_column_scale": jnp.clip(jnp.exp(math.log(2.0) - 1.3862944 * jax.random.uniform(arg_keys[8], (D,), jnp.float32) ** block_levels(arg_keys[8], (D,), ((0, 2),), -0.2, 0.2)), 0.5, 2.0),
        "premix_norm_gain": jnp.clip(1.0 + 0.18 * jax.random.normal(arg_keys[9], (D,), jnp.float32), 0.1, 1.9),
        "gate_matrix": gaussian(arg_keys[10], (D, FF), D ** -0.5, 0.125, ((0, 4), (1, 2)), jnp.float32),
        "gate_column_scale": jnp.clip(jnp.exp(math.log(2.0) - 1.3862944 * jax.random.uniform(arg_keys[11], (FF,), jnp.float32) ** block_levels(arg_keys[11], (FF,), ((0, 2),), -0.2, 0.2)), 0.5, 2.0),
        "up_matrix": gaussian(arg_keys[12], (D, FF), D ** -0.5, 0.125, ((0, 4), (1, 2)), jnp.float32),
        "up_column_scale": jnp.clip(jnp.exp(math.log(2.0) - 1.3862944 * jax.random.uniform(arg_keys[13], (FF,), jnp.float32) ** block_levels(arg_keys[13], (FF,), ((0, 2),), -0.2, 0.2)), 0.5, 2.0),
        "down_matrix": gaussian(arg_keys[14], (D, FF), FF ** -0.5, 0.109375, ((0, 4), (1, 2)), jnp.float32),
        "down_column_scale": jnp.clip(jnp.exp(math.log(2.0) - 1.3862944 * jax.random.uniform(arg_keys[15], (D,), jnp.float32) ** block_levels(arg_keys[15], (D,), ((0, 2),), -0.2, 0.2)), 0.5, 2.0),
    }


epsilon = 1e-06
softness_factor = 16.0
highest = lax.Precision.HIGHEST

def one_direction(query_heads, key_heads, value_heads, log_decay_values):
    sequence_batch, head_total, token_length, key_channel_width = query_heads.shape
    value_width = value_heads.shape[-1]
    block_count = token_length // BLOCK

    def blocks(tensor):
        return tensor.reshape(sequence_batch, head_total, block_count, BLOCK, tensor.shape[-1])
    q_blocks = blocks(query_heads)
    k_blocks = blocks(key_heads)
    v_blocks = blocks(value_heads)
    running = jnp.cumsum(blocks(log_decay_values), axis=3)
    block_end = running[:, :, :, -1:, :]
    q_dec = q_blocks * jnp.exp(running)
    k_inv = k_blocks * jnp.exp(-running)
    k_end = k_blocks * jnp.exp(block_end - running)
    lower_mask = jnp.tril(jnp.ones((BLOCK, BLOCK), jnp.float32))
    scores = jnp.einsum('shnid,shnjd->shnij', q_dec, k_inv, precision=highest) * lower_mask
    inner_part = jnp.einsum('shnij,shnje->shnie', scores, v_blocks, precision=highest)
    fading = jnp.exp(block_end[:, :, :, 0, :])

    def advance(memory, pieces):
        q_piece, k_piece, v_piece, f_piece = pieces
        carried = jnp.einsum('shcd,shde->shce', q_piece, memory, precision=highest)
        memory = f_piece[..., None] * memory + jnp.einsum('shcd,shce->shde', k_piece, v_piece, precision=highest)
        return (memory, carried)
    pieces = tuple((jnp.moveaxis(tensor, 2, 0) for tensor in (q_dec, k_end, v_blocks, fading)))
    initial = jnp.zeros((sequence_batch, head_total, key_channel_width, value_width), jnp.float32)
    _, carried = lax.scan(advance, initial, pieces)
    summed = inner_part + jnp.moveaxis(carried, 0, 2)
    return summed.reshape(sequence_batch, head_total, token_length, value_width)

def backwards(tensor):
    return tensor[:, :, ::-1]

def linear_attend(queries, key_matrix, value_matrix, decay_logodds, decay_surge, head_norm_gain):
    sequence_batch, token_length, head_total = decay_surge.shape
    key_channel_width = queries.shape[-1] // head_total
    value_width = value_matrix.shape[-1] // head_total

    def split_heads(tensor, width):
        return jnp.transpose(tensor.astype(jnp.float32).reshape(sequence_batch, token_length, head_total, width), (0, 2, 1, 3))
    query_heads = split_heads(queries, key_channel_width) * key_channel_width ** (-0.5)
    key_heads = split_heads(key_matrix, key_channel_width)
    value_heads = split_heads(value_matrix, value_width)
    gate_values = jax.nn.log_sigmoid(decay_logodds).reshape(sequence_batch, token_length, head_total, key_channel_width) / softness_factor
    log_decay_values = jnp.transpose(gate_values + decay_surge[..., None], (0, 2, 1, 3))
    forward = one_direction(query_heads, key_heads, value_heads, log_decay_values)
    backward = backwards(one_direction(backwards(query_heads), backwards(key_heads), backwards(value_heads), backwards(log_decay_values)))
    attended = forward + backward
    scaled = attended * lax.rsqrt(lax.optimization_barrier(jnp.mean(attended * attended, axis=-1, keepdims=True)) + epsilon) * head_norm_gain
    merged = jnp.transpose(scaled, (0, 2, 1, 3)).reshape(sequence_batch * token_length, head_total * value_width)
    return merged.astype(jnp.bfloat16)

def grouped(left, right):
    width = left.shape[1] // N_TP
    left_parts = left.reshape(left.shape[0], N_TP, width).astype(jnp.float32)
    right_parts = right.reshape(right.shape[0], N_TP, width).astype(jnp.float32)
    terms = jnp.einsum('lgc,dgc->gld', left_parts, right_parts, precision=highest)
    rounded = lax.optimization_barrier(terms.astype(jnp.bfloat16))
    return lax.optimization_barrier(jnp.sum(rounded.astype(jnp.float32), axis=0))

def rms_scaled(rows_in, gain):
    wide_rows = rows_in.astype(jnp.float32)
    factor = lax.rsqrt(lax.optimization_barrier(jnp.mean(wide_rows * wide_rows, axis=-1, keepdims=True)) + epsilon)
    return (wide_rows * factor * gain).astype(jnp.bfloat16)

def reference(residual, queries, key_matrix, value_matrix, decay_logodds, decay_surge, head_norm_gain, output_matrix, output_column_scale, premix_norm_gain, gate_matrix, gate_column_scale, up_matrix, up_column_scale, down_matrix, down_column_scale):
    out_half = output_matrix.astype(jnp.bfloat16)
    gate_half = gate_matrix.astype(jnp.bfloat16)
    up_half = up_matrix.astype(jnp.bfloat16)
    down_half = down_matrix.astype(jnp.bfloat16)

    def single_sequence(input_rows):
        residual_sequence, query_sequence, key_sequence, value_sequence, logodds_sequence, surge_sequence = input_rows
        normalized_rows = linear_attend(query_sequence[None], key_sequence[None], value_sequence[None], logodds_sequence[None], surge_sequence[None], head_norm_gain)
        mix_total = grouped(normalized_rows, out_half)
        updated = (residual_sequence.astype(jnp.float32) + output_column_scale * mix_total).astype(jnp.bfloat16)
        normin = rms_scaled(updated, premix_norm_gain)
        gate_pre = jnp.dot(normin, gate_half, preferred_element_type=jnp.float32) * gate_column_scale
        up_pre = jnp.dot(normin, up_half, preferred_element_type=jnp.float32) * up_column_scale
        hidden = (jax.nn.silu(gate_pre) * up_pre).astype(jnp.bfloat16)
        down_total = grouped(hidden, down_half)
        return (updated.astype(jnp.float32) + down_column_scale * down_total).astype(jnp.bfloat16)
    return lax.map(single_sequence, (residual, queries, key_matrix, value_matrix, decay_logodds, decay_surge))
```

```python
import functools

import jax
import jax.numpy as jnp
from jax import lax
from jax.experimental import pallas as pl
from jax.experimental.pallas import tpu as pltpu
from jax.sharding import PartitionSpec as P

BLOCK = 64


epsilon = 1e-06
softness_factor = 16.0
highest = lax.Precision.HIGHEST


def attend_head(q, k, v, logodds, surge, gain):
    tokens, width = q.shape
    blocks = tokens // BLOCK
    mid = BLOCK // 2 - 1
    decay = (
        jnp.minimum(logodds, 0.0) - jnp.log1p(jnp.exp(-jnp.abs(logodds)))
    ) * (1.0 / softness_factor) + surge
    row = lax.broadcasted_iota(jnp.int32, (BLOCK, BLOCK), 0)
    col = lax.broadcasted_iota(jnp.int32, (BLOCK, BLOCK), 1)
    tri = jnp.where(row >= col, 1.0, 0.0).astype(jnp.bfloat16)
    q = q.astype(jnp.float32) * width ** (-0.5)
    k = k.astype(jnp.float32)
    high = decay.astype(jnp.bfloat16)
    low = (decay - high.astype(jnp.float32)).astype(jnp.bfloat16)
    pieces = []
    for n in range(blocks):
        rows = slice(n * BLOCK, (n + 1) * BLOCK)
        running = jnp.dot(tri, high[rows], preferred_element_type=jnp.float32) + jnp.dot(
            tri, low[rows], preferred_element_type=jnp.float32
        )
        before = running - decay[rows]
        center = running[mid : mid + 1]
        end = running[BLOCK - 1 : BLOCK]
        to_center = jnp.exp(center)
        from_center = jnp.exp(end - center)
        q_forward = q[rows] * jnp.exp(running - center)
        k_forward = k[rows] * jnp.exp(center - running)
        q_backward = q[rows] * jnp.exp(center - before)
        k_backward = k[rows] * jnp.exp(before - center)
        half = jnp.bfloat16
        scores = jnp.where(
            row >= col, by_rows(q_forward.astype(half), k_forward.astype(half)), 0.0
        ) + jnp.where(row <= col, by_rows(q_backward.astype(half), k_backward.astype(half)), 0.0)
        inner = jnp.dot(scores.astype(half), v[rows], preferred_element_type=jnp.float32)
        pieces.append(
            (
                inner,
                (q_forward * to_center).astype(half),
                (q_backward * from_center).astype(half),
                by_columns(v[rows], (k_forward * from_center).astype(half)),
                by_columns(v[rows], (k_backward * to_center).astype(half)),
                jnp.exp(end),
            )
        )
    totals = [piece[0] for piece in pieces]
    state = None
    for n in range(blocks):
        if state is not None:
            totals[n] = totals[n] + by_rows(pieces[n][1], state.astype(jnp.bfloat16))
        state = pieces[n][3] if state is None else pieces[n][5] * state + pieces[n][3]
    state = None
    for n in reversed(range(blocks)):
        if state is not None:
            totals[n] = totals[n] + by_rows(pieces[n][2], state.astype(jnp.bfloat16))
        state = pieces[n][4] if state is None else pieces[n][5] * state + pieces[n][4]
    attended = jnp.concatenate(totals, axis=0)
    scale = lax.rsqrt(jnp.mean(attended * attended, axis=-1, keepdims=True) + epsilon)
    return (attended * scale * gain).astype(jnp.bfloat16)


def by_columns(left, right):
    return lax.dot_general(
        left, right, (((0,), (0,)), ((), ())), preferred_element_type=jnp.float32
    )


def attend_kernel(head_total, q_ref, k_ref, v_ref, lo_ref, sg_ref, gain_ref, out_ref):
    width = q_ref.shape[1] // head_total
    value_width = v_ref.shape[1] // head_total
    for h in range(head_total):
        keys = slice(h * width, (h + 1) * width)
        values = slice(h * value_width, (h + 1) * value_width)
        out_ref[:, values] = attend_head(
            q_ref[:, keys],
            k_ref[:, keys],
            v_ref[:, values],
            lo_ref[:, keys],
            sg_ref[:, h : h + 1],
            gain_ref[...],
        )


def linear_attend(queries, key_matrix, value_matrix, decay_logodds, decay_surge, head_norm_gain):
    _, token_length, head_total = decay_surge.shape
    outs = [
        pl.pallas_call(
            functools.partial(attend_kernel, head_total),
            out_shape=jax.ShapeDtypeStruct(value_matrix.shape[1:], jnp.bfloat16),
            in_specs=[pl.BlockSpec(memory_space=pltpu.VMEM)] * 6,
            out_specs=pl.BlockSpec(memory_space=pltpu.VMEM),
            cost_estimate=pl.CostEstimate(
                flops=10**9, bytes_accessed=4 * 10**6, transcendentals=10**6
            ),
        )(
            queries[b], key_matrix[b], value_matrix[b], decay_logodds[b], decay_surge[b],
            head_norm_gain.reshape(1, -1),
        )
        for b in range(queries.shape[0])
    ]
    return jnp.concatenate(outs, axis=0)


def by_rows(left, right):
    return lax.dot_general(
        left, right, (((1,), (1,)), ((), ())), preferred_element_type=jnp.float32
    )


def body(
    residual,
    queries,
    key_matrix,
    value_matrix,
    decay_logodds,
    decay_surge,
    head_norm_gain,
    output_matrix,
    output_column_scale,
    premix_norm_gain,
    gate_matrix,
    gate_column_scale,
    up_matrix,
    up_column_scale,
    down_matrix,
    down_column_scale,
):
    sequence_batch, token_length, local_width = residual.shape
    row_count = sequence_batch * token_length
    normalized_rows = linear_attend(
        queries, key_matrix, value_matrix, decay_logodds, decay_surge, head_norm_gain
    )
    out_half = output_matrix.astype(jnp.bfloat16)
    out_full = lax.all_gather(out_half, "fs", axis=0, tiled=True)
    mix_terms = by_rows(normalized_rows, out_full)
    mix_total = lax.psum_scatter(
        mix_terms.astype(jnp.bfloat16), "tp", scatter_dimension=1, tiled=True
    ).astype(jnp.float32)
    own_rows = residual.reshape(row_count, local_width).astype(jnp.float32)
    updated = (own_rows + output_column_scale * mix_total).astype(jnp.bfloat16)
    features = lax.all_gather(updated, "tp", axis=1, tiled=True)
    wide_rows = features.astype(jnp.float32)
    factor = lax.rsqrt(jnp.mean(wide_rows * wide_rows, axis=-1, keepdims=True) + epsilon)
    normin = (wide_rows * factor * premix_norm_gain).astype(jnp.bfloat16)
    gate_half = gate_matrix.astype(jnp.bfloat16)
    up_half = up_matrix.astype(jnp.bfloat16)
    down_half = down_matrix.astype(jnp.bfloat16)
    gate_full, up_full, down_full = (
        lax.all_gather(gate_half, "fs", axis=0, tiled=True),
        lax.all_gather(up_half, "fs", axis=0, tiled=True),
        lax.all_gather(down_half, "fs", axis=0, tiled=True),
    )
    gate_pre = jnp.dot(normin, gate_full, preferred_element_type=jnp.float32)
    up_pre = jnp.dot(normin, up_full, preferred_element_type=jnp.float32)
    hidden = (jax.nn.silu(gate_pre * gate_column_scale) * (up_pre * up_column_scale)).astype(
        jnp.bfloat16
    )
    down_terms = by_rows(hidden, down_full)
    down_total = lax.psum_scatter(
        down_terms.astype(jnp.bfloat16), "tp", scatter_dimension=1, tiled=True
    ).astype(jnp.float32)
    result = (updated.astype(jnp.float32) + down_column_scale * down_total).astype(jnp.bfloat16)
    return result.reshape(sequence_batch, token_length, local_width)


def solution(mesh):
    return jax.shard_map(
        body,
        mesh=mesh,
        in_specs=(
            P(("rep", "fs"), None, "tp"),
            P(("rep", "fs"), None, "tp"),
            P(("rep", "fs"), None, "tp"),
            P(("rep", "fs"), None, "tp"),
            P(("rep", "fs"), None, "tp"),
            P(("rep", "fs"), None, "tp"),
            P(),
            P("fs", "tp"),
            P("tp"),
            P(),
            P("fs", "tp"),
            P("tp"),
            P("fs", "tp"),
            P("tp"),
            P("fs", "tp"),
            P("tp"),
        ),
        out_specs=P(("rep", "fs"), None, "tp"),
        check_vma=False,
    )
```

```python
import functools

import jax
import jax.numpy as jnp
from jax import lax
from jax.experimental import pallas as pl
from jax.experimental.pallas import tpu as pltpu
from jax.sharding import PartitionSpec as P

BLOCK = 64


epsilon = 1e-06
softness_factor = 16.0
highest = lax.Precision.HIGHEST


def attend_head(q, k, v, logodds, surge, gain):
    tokens, width = q.shape
    blocks = tokens // BLOCK
    mid = BLOCK // 2 - 1
    decay = (
        jnp.minimum(logodds, 0.0) - jnp.log1p(jnp.exp(-jnp.abs(logodds)))
    ) * (1.0 / softness_factor) + surge
    row = lax.broadcasted_iota(jnp.int32, (BLOCK, BLOCK), 0)
    col = lax.broadcasted_iota(jnp.int32, (BLOCK, BLOCK), 1)
    tri = jnp.where(row >= col, 1.0, 0.0).astype(jnp.bfloat16)
    q = q.astype(jnp.float32) * width ** (-0.5)
    k = k.astype(jnp.float32)
    high = decay.astype(jnp.bfloat16)
    low = (decay - high.astype(jnp.float32)).astype(jnp.bfloat16)
    pieces = []
    for n in range(blocks):
        rows = slice(n * BLOCK, (n + 1) * BLOCK)
        running = jnp.dot(tri, high[rows], preferred_element_type=jnp.float32) + jnp.dot(
            tri, low[rows], preferred_element_type=jnp.float32
        )
        before = running - decay[rows]
        center = running[mid : mid + 1]
        end = running[BLOCK - 1 : BLOCK]
        to_center = jnp.exp(center)
        from_center = jnp.exp(end - center)
        q_forward = q[rows] * jnp.exp(running - center)
        k_forward = k[rows] * jnp.exp(center - running)
        q_backward = q[rows] * jnp.exp(center - before)
        k_backward = k[rows] * jnp.exp(before - center)
        half = jnp.bfloat16
        scores = jnp.where(
            row >= col, by_rows(q_forward.astype(half), k_forward.astype(half)), 0.0
        ) + jnp.where(row <= col, by_rows(q_backward.astype(half), k_backward.astype(half)), 0.0)
        inner = jnp.dot(scores.astype(half), v[rows], preferred_element_type=jnp.float32)
        pieces.append(
            (
                inner,
                (q_forward * to_center).astype(half),
                (q_backward * from_center).astype(half),
                by_columns(v[rows], (k_forward * from_center).astype(half)),
                by_columns(v[rows], (k_backward * to_center).astype(half)),
                jnp.exp(end),
            )
        )
    totals = [piece[0] for piece in pieces]
    state = None
    for n in range(blocks):
        if state is not None:
            totals[n] = totals[n] + by_rows(pieces[n][1], state.astype(jnp.bfloat16))
        state = pieces[n][3] if state is None else pieces[n][5] * state + pieces[n][3]
    state = None
    for n in reversed(range(blocks)):
        if state is not None:
            totals[n] = totals[n] + by_rows(pieces[n][2], state.astype(jnp.bfloat16))
        state = pieces[n][4] if state is None else pieces[n][5] * state + pieces[n][4]
    attended = jnp.concatenate(totals, axis=0)
    scale = lax.rsqrt(jnp.mean(attended * attended, axis=-1, keepdims=True) + epsilon)
    return (attended * scale * gain).astype(jnp.bfloat16)


def by_columns(left, right):
    return lax.dot_general(
        left, right, (((0,), (0,)), ((), ())), preferred_element_type=jnp.float32
    )


def attend_kernel(head_total, q_ref, k_ref, v_ref, lo_ref, sg_ref, gain_ref, out_ref):
    width = q_ref.shape[1] // head_total
    value_width = v_ref.shape[1] // head_total
    for h in range(head_total):
        keys = slice(h * width, (h + 1) * width)
        values = slice(h * value_width, (h + 1) * value_width)
        out_ref[:, values] = attend_head(
            q_ref[:, keys],
            k_ref[:, keys],
            v_ref[:, values],
            lo_ref[:, keys],
            sg_ref[:, h : h + 1],
            gain_ref[...],
        )


def linear_attend(queries, key_matrix, value_matrix, decay_logodds, decay_surge, head_norm_gain):
    _, token_length, head_total = decay_surge.shape
    outs = [
        pl.pallas_call(
            functools.partial(attend_kernel, head_total),
            out_shape=jax.ShapeDtypeStruct(value_matrix.shape[1:], jnp.bfloat16),
            in_specs=[pl.BlockSpec(memory_space=pltpu.VMEM)] * 6,
            out_specs=pl.BlockSpec(memory_space=pltpu.VMEM),
            cost_estimate=pl.CostEstimate(
                flops=10**9, bytes_accessed=4 * 10**6, transcendentals=10**6
            ),
        )(
            queries[b], key_matrix[b], value_matrix[b], decay_logodds[b], decay_surge[b],
            head_norm_gain.reshape(1, -1),
        )
        for b in range(queries.shape[0])
    ]
    return jnp.concatenate(outs, axis=0)


def by_rows(left, right):
    return lax.dot_general(
        left, right, (((1,), (1,)), ((), ())), preferred_element_type=jnp.float32
    )


def body(
    residual,
    queries,
    key_matrix,
    value_matrix,
    decay_logodds,
    decay_surge,
    head_norm_gain,
    output_matrix,
    output_column_scale,
    premix_norm_gain,
    gate_matrix,
    gate_column_scale,
    up_matrix,
    up_column_scale,
    down_matrix,
    down_column_scale,
):
    sequence_batch, token_length, local_width = residual.shape
    row_count = sequence_batch * token_length
    normalized_rows = linear_attend(
        queries, key_matrix, value_matrix, decay_logodds, decay_surge, head_norm_gain
    )
    out_half = output_matrix.astype(jnp.bfloat16)
    out_full = lax.all_gather(out_half, "fs", axis=0, tiled=True)
    mix_terms = by_rows(normalized_rows, out_full)
    mix_total = lax.psum_scatter(
        mix_terms.astype(jnp.bfloat16), "tp", scatter_dimension=1, tiled=True
    ).astype(jnp.float32)
    own_rows = residual.reshape(row_count, local_width).astype(jnp.float32)
    updated = (own_rows + output_column_scale * mix_total).astype(jnp.bfloat16)
    features = lax.all_gather(updated, "tp", axis=1, tiled=True)
    wide_rows = features.astype(jnp.float32)
    factor = lax.rsqrt(jnp.mean(wide_rows * wide_rows, axis=-1, keepdims=True) + epsilon)
    normin = (wide_rows * factor * premix_norm_gain).astype(jnp.bfloat16)
    gate_half = gate_matrix.astype(jnp.bfloat16)
    up_half = up_matrix.astype(jnp.bfloat16)
    down_half = down_matrix.astype(jnp.bfloat16)
    gate_full, up_full, down_full = (
        lax.all_gather(gate_half, "fs", axis=0, tiled=True),
        lax.all_gather(up_half, "fs", axis=0, tiled=True),
        lax.all_gather(down_half, "fs", axis=0, tiled=True),
    )
    gate_pre = jnp.dot(normin, gate_full, preferred_element_type=jnp.float32)
    up_pre = jnp.dot(normin, up_full, preferred_element_type=jnp.float32)
    hidden = (jax.nn.silu(gate_pre * gate_column_scale) * (up_pre * up_column_scale)).astype(
        jnp.bfloat16
    )
    down_terms = by_rows(hidden, down_full)
    down_total = lax.psum_scatter(
        down_terms.astype(jnp.bfloat16), "tp", scatter_dimension=1, tiled=True
    ).astype(jnp.float32)
    result = (updated.astype(jnp.float32) + down_column_scale * down_total).astype(jnp.bfloat16)
    return result.reshape(sequence_batch, token_length, local_width)


def exchange_kernel(axis, n, spread, count, *refs):
    ins, outs = refs[:count], refs[count : 2 * count]
    send_sem, recv_sem = refs[2 * count :]
    me = lax.axis_index(axis)
    barrier = pltpu.get_barrier_semaphore()
    for step in range(1, n):
        pl.semaphore_signal(
            barrier,
            inc=1,
            device_id={axis: lax.rem(me + step, n)},
            device_id_type=pl.DeviceIdType.MESH,
        )
    pl.semaphore_wait(barrier, n - 1)
    copies = []
    for step in range(1, n):
        peer = lax.rem(me + step, n)
        for c in range(count):
            copy = pltpu.make_async_remote_copy(
                src_ref=ins[c].at[peer] if spread else ins[c],
                dst_ref=outs[c].at[me],
                send_sem=send_sem.at[c, step - 1],
                recv_sem=recv_sem.at[c, step - 1],
                device_id={axis: peer},
                device_id_type=pl.DeviceIdType.MESH,
            )
            copy.start()
            copies.append(copy)
    for c in range(count):
        outs[c][me] = ins[c][me] if spread else ins[c][...]
    for copy in copies:
        copy.wait()


def exchange(arrays, axis, n, spread, call):
    count = len(arrays)
    shapes = [a.shape if spread else (n,) + a.shape for a in arrays]
    return pl.pallas_call(
        functools.partial(exchange_kernel, axis, n, spread, count),
        out_shape=[jax.ShapeDtypeStruct(d, a.dtype) for d, a in zip(shapes, arrays)],
        in_specs=[pl.BlockSpec(memory_space=pltpu.VMEM)] * count,
        out_specs=[pl.BlockSpec(memory_space=pltpu.VMEM)] * count,
        scratch_shapes=[
            pltpu.SemaphoreType.DMA((count, n - 1)),
            pltpu.SemaphoreType.DMA((count, n - 1)),
        ],
        compiler_params=pltpu.CompilerParams(collective_id=call, has_side_effects=True),
        cost_estimate=pl.CostEstimate(
            flops=10**9, bytes_accessed=2 * 10**7, transcendentals=0
        ),
    )(*arrays)


def moving_body(
    sizes,
    residual,
    queries,
    key_matrix,
    value_matrix,
    decay_logodds,
    decay_surge,
    head_norm_gain,
    output_matrix,
    output_column_scale,
    premix_norm_gain,
    gate_matrix,
    gate_column_scale,
    up_matrix,
    up_column_scale,
    down_matrix,
    down_column_scale,
):
    n_rep, n_fs, n_tp = sizes
    half = jnp.bfloat16
    sequence_batch, token_length, local_width = residual.shape
    row_count = sequence_batch * token_length
    width = local_width * n_tp
    own_width = output_matrix.shape[0]
    part = own_width // n_tp
    units = gate_matrix.shape[1] // n_fs
    padded = -(-units // 128) * 128
    slab = own_width // n_rep
    rep, fs, tp = lax.axis_index("rep"), lax.axis_index("fs"), lax.axis_index("tp")

    def slabs(matrix):
        rows = lax.dynamic_slice_in_dim(matrix, rep * slab, slab, axis=0).astype(half)
        rows = jnp.pad(rows.reshape(slab, n_fs, units), ((0, 0), (0, 0), (0, padded - units)))
        return jnp.transpose(rows, (1, 0, 2))

    weights = jnp.concatenate([slabs(m) for m in (gate_matrix, up_matrix, down_matrix)], axis=2)
    own_rows = residual.reshape(row_count, local_width)
    both_rows, both_scale = exchange(
        [own_rows, output_column_scale.reshape(1, local_width)], "tp", n_tp, False, 1
    )
    wide = jnp.transpose(both_rows, (1, 0, 2)).reshape(row_count, n_fs, n_tp, part)
    mine = lax.dynamic_index_in_dim(wide, tp, axis=2, keepdims=False)
    got_weights, got_rows = exchange(
        [weights, jnp.transpose(mine, (1, 0, 2))], "fs", n_fs, True, 2
    )
    all_weights = lax.all_gather(got_weights, "rep", axis=0, tiled=False)
    all_weights = jnp.transpose(all_weights, (1, 0, 2, 3)).reshape(width, 3 * padded)

    normalized_rows = linear_attend(
        queries, key_matrix, value_matrix, decay_logodds, decay_surge, head_norm_gain
    )
    (gathered,) = exchange([normalized_rows], "fs", n_fs, False, 3)
    group_rows = n_fs * row_count
    mix_terms = by_rows(gathered.reshape(group_rows, -1), output_matrix.astype(half)).astype(half)
    mix_split = jnp.transpose(mix_terms.reshape(group_rows, n_tp, part), (1, 0, 2))
    (mix_parts,) = exchange([mix_split], "tp", n_tp, True, 4)
    mixed = jnp.sum(mix_parts.astype(jnp.float32), axis=0)
    out_scale = lax.dynamic_index_in_dim(
        lax.dynamic_index_in_dim(both_scale.reshape(n_fs, n_tp, part), fs, 0, False), tp, 0, False
    )
    piece = got_rows.reshape(group_rows, part).astype(jnp.float32) + out_scale * mixed
    (over_fs,) = exchange([piece.astype(half)], "fs", n_fs, False, 5)
    (over_tp,) = exchange([over_fs], "tp", n_tp, False, 6)
    updated = jnp.transpose(over_tp, (2, 1, 0, 3)).reshape(group_rows, width)
    wide_rows = updated.astype(jnp.float32)
    factor = lax.rsqrt(jnp.mean(wide_rows * wide_rows, axis=-1, keepdims=True) + epsilon)
    normin = (wide_rows * factor * premix_norm_gain).astype(half)

    def unit_scale(scale):
        own = lax.dynamic_index_in_dim(scale.reshape(n_fs, units), fs, 0, False)
        return jnp.pad(own, (0, padded - units))

    both = jnp.dot(normin, all_weights[:, : 2 * padded], preferred_element_type=jnp.float32)
    gate_pre = both[:, :padded] * unit_scale(gate_column_scale)
    up_pre = both[:, padded:] * unit_scale(up_column_scale)
    hidden = (jax.nn.silu(gate_pre) * up_pre).astype(half)
    down_terms = jnp.concatenate(
        [
            by_rows(
                hidden, all_weights[t * local_width : (t + 1) * local_width, 2 * padded :]
            ).astype(half)[None]
            for t in range(n_tp)
        ],
        axis=0,
    )
    (down_parts,) = exchange([down_terms], "tp", n_tp, True, 7)
    down_half = jnp.sum(down_parts.astype(jnp.float32), axis=0).astype(half)
    (down_back,) = exchange(
        [down_half.reshape(n_fs, row_count, local_width)], "fs", n_fs, True, 8
    )
    down_total = jnp.sum(down_back.astype(jnp.float32), axis=0)
    own_updated = lax.dynamic_slice(
        updated, (fs * row_count, tp * local_width), (row_count, local_width)
    )
    result = (own_updated.astype(jnp.float32) + down_column_scale * down_total).astype(half)
    return result.reshape(sequence_batch, token_length, local_width)


def chosen_body(mesh):
    sizes = tuple(mesh.shape[name] for name in ("rep", "fs", "tp"))
    n_rep, n_fs, n_tp = sizes

    def run(*args):
        residual, output_matrix, gate_matrix = args[0], args[7], args[10]
        weights = output_matrix.size + 3 * gate_matrix.size
        rows = residual.shape[0] * residual.shape[1]
        moved = 3 * rows * residual.shape[2] + 3 * gate_matrix.size // n_rep
        fits = (
            n_fs > 1
            and n_tp > 1
            and output_matrix.shape[0] % (128 * n_tp) == 0
            and output_matrix.shape[0] % (16 * n_rep) == 0
        )
        if fits and moved < weights:
            return moving_body(sizes, *args)
        return body(*args)

    return run


def solution(mesh):
    return jax.shard_map(
        chosen_body(mesh),
        mesh=mesh,
        in_specs=(
            P(("rep", "fs"), None, "tp"),
            P(("rep", "fs"), None, "tp"),
            P(("rep", "fs"), None, "tp"),
            P(("rep", "fs"), None, "tp"),
            P(("rep", "fs"), None, "tp"),
            P(("rep", "fs"), None, "tp"),
            P(),
            P("fs", "tp"),
            P("tp"),
            P(),
            P("fs", "tp"),
            P("tp"),
            P("fs", "tp"),
            P("tp"),
            P("fs", "tp"),
            P("tp"),
        ),
        out_specs=P(("rep", "fs"), None, "tp"),
        check_vma=False,
    )
```

```python
import functools

import jax
import jax.numpy as jnp
from jax import lax
from jax.experimental import pallas as pl
from jax.experimental.pallas import tpu as pltpu
from jax.sharding import PartitionSpec as P

BLOCK = 64


epsilon = 1e-06
softness_factor = 16.0
highest = lax.Precision.HIGHEST


def attend_head(q, k, v, logodds, surge, gain):
    tokens, width = q.shape
    blocks = tokens // BLOCK
    mid = BLOCK // 2 - 1
    decay = (
        jnp.minimum(logodds, 0.0) - jnp.log1p(jnp.exp(-jnp.abs(logodds)))
    ) * (1.0 / softness_factor) + surge
    row = lax.broadcasted_iota(jnp.int32, (BLOCK, BLOCK), 0)
    col = lax.broadcasted_iota(jnp.int32, (BLOCK, BLOCK), 1)
    tri = jnp.where(row >= col, 1.0, 0.0).astype(jnp.bfloat16)
    q = q.astype(jnp.float32) * width ** (-0.5)
    k = k.astype(jnp.float32)
    high = decay.astype(jnp.bfloat16)
    low = (decay - high.astype(jnp.float32)).astype(jnp.bfloat16)
    pieces = []
    for n in range(blocks):
        rows = slice(n * BLOCK, (n + 1) * BLOCK)
        running = jnp.dot(tri, high[rows], preferred_element_type=jnp.float32) + jnp.dot(
            tri, low[rows], preferred_element_type=jnp.float32
        )
        before = running - decay[rows]
        center = running[mid : mid + 1]
        end = running[BLOCK - 1 : BLOCK]
        to_center = jnp.exp(center)
        from_center = jnp.exp(end - center)
        q_forward = q[rows] * jnp.exp(running - center)
        k_forward = k[rows] * jnp.exp(center - running)
        q_backward = q[rows] * jnp.exp(center - before)
        k_backward = k[rows] * jnp.exp(before - center)
        half = jnp.bfloat16
        scores = jnp.where(
            row >= col, by_rows(q_forward.astype(half), k_forward.astype(half)), 0.0
        ) + jnp.where(row <= col, by_rows(q_backward.astype(half), k_backward.astype(half)), 0.0)
        inner = jnp.dot(scores.astype(half), v[rows], preferred_element_type=jnp.float32)
        pieces.append(
            (
                inner,
                (q_forward * to_center).astype(half),
                (q_backward * from_center).astype(half),
                by_columns(v[rows], (k_forward * from_center).astype(half)),
                by_columns(v[rows], (k_backward * to_center).astype(half)),
                jnp.exp(end),
            )
        )
    totals = [piece[0] for piece in pieces]
    state = None
    for n in range(blocks):
        if state is not None:
            totals[n] = totals[n] + by_rows(pieces[n][1], state.astype(jnp.bfloat16))
        state = pieces[n][3] if state is None else pieces[n][5] * state + pieces[n][3]
    state = None
    for n in reversed(range(blocks)):
        if state is not None:
            totals[n] = totals[n] + by_rows(pieces[n][2], state.astype(jnp.bfloat16))
        state = pieces[n][4] if state is None else pieces[n][5] * state + pieces[n][4]
    attended = jnp.concatenate(totals, axis=0)
    scale = lax.rsqrt(jnp.mean(attended * attended, axis=-1, keepdims=True) + epsilon)
    return (attended * scale * gain).astype(jnp.bfloat16)


def by_columns(left, right):
    return lax.dot_general(
        left, right, (((0,), (0,)), ((), ())), preferred_element_type=jnp.float32
    )


def attend_kernel(head_total, q_ref, k_ref, v_ref, lo_ref, sg_ref, gain_ref, out_ref):
    width = q_ref.shape[1] // head_total
    value_width = v_ref.shape[1] // head_total
    for h in range(head_total):
        keys = slice(h * width, (h + 1) * width)
        values = slice(h * value_width, (h + 1) * value_width)
        out_ref[:, values] = attend_head(
            q_ref[:, keys],
            k_ref[:, keys],
            v_ref[:, values],
            lo_ref[:, keys],
            sg_ref[:, h : h + 1],
            gain_ref[...],
        )


def linear_attend(queries, key_matrix, value_matrix, decay_logodds, decay_surge, head_norm_gain):
    _, token_length, head_total = decay_surge.shape
    outs = [
        pl.pallas_call(
            functools.partial(attend_kernel, head_total),
            out_shape=jax.ShapeDtypeStruct(value_matrix.shape[1:], jnp.bfloat16),
            in_specs=[pl.BlockSpec(memory_space=pltpu.VMEM)] * 6,
            out_specs=pl.BlockSpec(memory_space=pltpu.VMEM),
            cost_estimate=pl.CostEstimate(
                flops=10**9, bytes_accessed=4 * 10**6, transcendentals=10**6
            ),
        )(
            queries[b], key_matrix[b], value_matrix[b], decay_logodds[b], decay_surge[b],
            head_norm_gain.reshape(1, -1),
        )
        for b in range(queries.shape[0])
    ]
    return jnp.concatenate(outs, axis=0)


def by_rows(left, right):
    return lax.dot_general(
        left, right, (((1,), (1,)), ((), ())), preferred_element_type=jnp.float32
    )


def body(
    residual,
    queries,
    key_matrix,
    value_matrix,
    decay_logodds,
    decay_surge,
    head_norm_gain,
    output_matrix,
    output_column_scale,
    premix_norm_gain,
    gate_matrix,
    gate_column_scale,
    up_matrix,
    up_column_scale,
    down_matrix,
    down_column_scale,
):
    sequence_batch, token_length, local_width = residual.shape
    row_count = sequence_batch * token_length
    normalized_rows = linear_attend(
        queries, key_matrix, value_matrix, decay_logodds, decay_surge, head_norm_gain
    )
    out_half = output_matrix.astype(jnp.bfloat16)
    out_full = lax.all_gather(out_half, "fs", axis=0, tiled=True)
    mix_terms = by_rows(normalized_rows, out_full)
    mix_total = lax.psum_scatter(
        mix_terms.astype(jnp.bfloat16), "tp", scatter_dimension=1, tiled=True
    ).astype(jnp.float32)
    own_rows = residual.reshape(row_count, local_width).astype(jnp.float32)
    updated = (own_rows + output_column_scale * mix_total).astype(jnp.bfloat16)
    features = lax.all_gather(updated, "tp", axis=1, tiled=True)
    wide_rows = features.astype(jnp.float32)
    factor = lax.rsqrt(jnp.mean(wide_rows * wide_rows, axis=-1, keepdims=True) + epsilon)
    normin = (wide_rows * factor * premix_norm_gain).astype(jnp.bfloat16)
    gate_half = gate_matrix.astype(jnp.bfloat16)
    up_half = up_matrix.astype(jnp.bfloat16)
    down_half = down_matrix.astype(jnp.bfloat16)
    gate_full, up_full, down_full = (
        lax.all_gather(gate_half, "fs", axis=0, tiled=True),
        lax.all_gather(up_half, "fs", axis=0, tiled=True),
        lax.all_gather(down_half, "fs", axis=0, tiled=True),
    )
    gate_pre = jnp.dot(normin, gate_full, preferred_element_type=jnp.float32)
    up_pre = jnp.dot(normin, up_full, preferred_element_type=jnp.float32)
    hidden = (jax.nn.silu(gate_pre * gate_column_scale) * (up_pre * up_column_scale)).astype(
        jnp.bfloat16
    )
    down_terms = by_rows(hidden, down_full)
    down_total = lax.psum_scatter(
        down_terms.astype(jnp.bfloat16), "tp", scatter_dimension=1, tiled=True
    ).astype(jnp.float32)
    result = (updated.astype(jnp.float32) + down_column_scale * down_total).astype(jnp.bfloat16)
    return result.reshape(sequence_batch, token_length, local_width)


def exchange_kernel(axis, n, spread, count, *refs):
    ins, outs = refs[:count], refs[count : 2 * count]
    send_sem, recv_sem = refs[2 * count :]
    me = lax.axis_index(axis)
    barrier = pltpu.get_barrier_semaphore()
    for step in range(1, n):
        pl.semaphore_signal(
            barrier,
            inc=1,
            device_id={axis: lax.rem(me + step, n)},
            device_id_type=pl.DeviceIdType.MESH,
        )
    pl.semaphore_wait(barrier, n - 1)
    copies = []
    for step in range(1, n):
        peer = lax.rem(me + step, n)
        for c in range(count):
            copy = pltpu.make_async_remote_copy(
                src_ref=ins[c].at[peer] if spread else ins[c],
                dst_ref=outs[c].at[me],
                send_sem=send_sem.at[c, step - 1],
                recv_sem=recv_sem.at[c, step - 1],
                device_id={axis: peer},
                device_id_type=pl.DeviceIdType.MESH,
            )
            copy.start()
            copies.append(copy)
    for c in range(count):
        outs[c][me] = ins[c][me] if spread else ins[c][...]
    for copy in copies:
        copy.wait()


def exchange(arrays, axis, n, spread, call):
    count = len(arrays)
    shapes = [a.shape if spread else (n,) + a.shape for a in arrays]
    return pl.pallas_call(
        functools.partial(exchange_kernel, axis, n, spread, count),
        out_shape=[jax.ShapeDtypeStruct(d, a.dtype) for d, a in zip(shapes, arrays)],
        in_specs=[pl.BlockSpec(memory_space=pltpu.VMEM)] * count,
        out_specs=[pl.BlockSpec(memory_space=pltpu.VMEM)] * count,
        scratch_shapes=[
            pltpu.SemaphoreType.DMA((count, n - 1)),
            pltpu.SemaphoreType.DMA((count, n - 1)),
        ],
        compiler_params=pltpu.CompilerParams(collective_id=call, has_side_effects=True),
        cost_estimate=pl.CostEstimate(
            flops=10**9, bytes_accessed=2 * 10**7, transcendentals=0
        ),
    )(*arrays)


def send(source, target, sems, index, device):
    copy = pltpu.make_async_remote_copy(
        src_ref=source,
        dst_ref=target,
        send_sem=sems[0].at[index],
        recv_sem=sems[1].at[index],
        device_id=device,
        device_id_type=pl.DeviceIdType.MESH,
    )
    copy.start()
    return copy


def greet(devices):
    barrier = pltpu.get_barrier_semaphore()
    for device in devices:
        pl.semaphore_signal(
            barrier, inc=1, device_id=device, device_id_type=pl.DeviceIdType.MESH
        )
    pl.semaphore_wait(barrier, len(devices))


def gather_kernel(share, x_ref, out_ref, *sems):
    me, tp = lax.axis_index("fs"), lax.axis_index("tp")
    near = me + 1 - 2 * lax.rem(me, 2)
    far = lax.rem(me + 2, 4)
    corner = lax.rem(near + 2, 4)
    to_near, to_far, to_pair = {"fs": near}, {"fs": far}, {"tp": 1 - tp}
    greet([to_near, to_far] + ([to_pair] if share else []))
    own = out_ref.at[tp] if share else out_ref
    rows = x_ref.shape[0] // 2
    upper, lower = pl.ds(0, rows), pl.ds(rows, rows)
    near_upper = send(x_ref.at[upper], own.at[me, upper], sems, 0, to_near)
    far_lower = send(x_ref.at[lower], own.at[me, lower], sems, 1, to_far)
    near_lower = send(x_ref.at[lower], own.at[me, lower], sems, 2, to_near)
    far_upper = send(x_ref.at[upper], own.at[me, upper], sems, 3, to_far)
    copies = [near_upper, far_lower, near_lower, far_upper]
    shared = [send(x_ref, own.at[me], sems, 6, to_pair)] if share else []
    own[me] = x_ref[...]
    near_upper.wait_recv()
    corner_upper = send(own.at[near, upper], own.at[near, upper], sems, 4, to_far)
    far_lower.wait_recv()
    corner_lower = send(own.at[far, lower], own.at[far, lower], sems, 5, to_near)
    near_lower.wait_recv()
    if share:
        shared.append(send(own.at[near], own.at[near], sems, 7, to_pair))
    far_upper.wait_recv()
    if share:
        shared.append(send(own.at[far], own.at[far], sems, 8, to_pair))
    corner_upper.wait_recv()
    corner_lower.wait_recv()
    if share:
        shared.append(send(own.at[corner], own.at[corner], sems, 9, to_pair))
    for copy in copies + [corner_upper, corner_lower]:
        copy.wait_send()
    for copy in shared:
        copy.wait()


def gather(x, n_fs, n_tp, share, call):
    shape = ((n_tp,) if share else ()) + (n_fs,) + x.shape
    return pl.pallas_call(
        functools.partial(gather_kernel, share),
        out_shape=jax.ShapeDtypeStruct(shape, x.dtype),
        in_specs=[pl.BlockSpec(memory_space=pltpu.VMEM)],
        out_specs=pl.BlockSpec(memory_space=pltpu.VMEM),
        scratch_shapes=[pltpu.SemaphoreType.DMA((10,)), pltpu.SemaphoreType.DMA((10,))],
        compiler_params=pltpu.CompilerParams(collective_id=call, has_side_effects=True),
        cost_estimate=pl.CostEstimate(
            flops=10**9, bytes_accessed=2 * 10**7, transcendentals=0
        ),
    )(x)


def reduce_kernel(n, terms_ref, back_ref, part_ref, total_ref, *sems):
    me, tp = lax.axis_index("fs"), lax.axis_index("tp")
    steps = list(range(1, n)) + [0]
    peers = [lax.rem(me + step, n) for step in range(n)]
    greet([{"fs": peers[step]} for step in range(1, n)] + [{"tp": 1 - tp}])
    pairs = {
        step: send(
            terms_ref.at[1 - tp, peers[step]], part_ref.at[peers[step]], sems, step, {"tp": 1 - tp}
        )
        for step in steps
    }
    copies = []
    for step in steps:
        peer = peers[step]
        pairs[step].wait_recv()
        total = terms_ref[tp, peer].astype(jnp.float32) + part_ref[peer].astype(jnp.float32)
        if step == 0:
            back_ref[me] = total.astype(back_ref.dtype)
        else:
            total_ref[peer] = total.astype(back_ref.dtype)
            copies.append(
                send(total_ref.at[peer], back_ref.at[me], sems, n + step, {"fs": peer})
            )
    for step in steps:
        pairs[step].wait_send()
    for copy in copies:
        copy.wait()


def reduce_back(terms, n_fs, call):
    shape = terms.shape[1:]
    return pl.pallas_call(
        functools.partial(reduce_kernel, n_fs),
        out_shape=jax.ShapeDtypeStruct(shape, terms.dtype),
        in_specs=[pl.BlockSpec(memory_space=pltpu.VMEM)],
        out_specs=pl.BlockSpec(memory_space=pltpu.VMEM),
        scratch_shapes=[
            pltpu.VMEM(shape, terms.dtype),
            pltpu.VMEM(shape, terms.dtype),
            pltpu.SemaphoreType.DMA((2 * n_fs,)),
            pltpu.SemaphoreType.DMA((2 * n_fs,)),
        ],
        compiler_params=pltpu.CompilerParams(collective_id=call, has_side_effects=True),
        cost_estimate=pl.CostEstimate(
            flops=10**9, bytes_accessed=2 * 10**7, transcendentals=0
        ),
    )(terms)


def moving_body(
    sizes,
    residual,
    queries,
    key_matrix,
    value_matrix,
    decay_logodds,
    decay_surge,
    head_norm_gain,
    output_matrix,
    output_column_scale,
    premix_norm_gain,
    gate_matrix,
    gate_column_scale,
    up_matrix,
    up_column_scale,
    down_matrix,
    down_column_scale,
):
    n_rep, n_fs, n_tp = sizes
    half = jnp.bfloat16
    sequence_batch, token_length, local_width = residual.shape
    row_count = sequence_batch * token_length
    width = local_width * n_tp
    own_width = output_matrix.shape[0]
    part = own_width // n_tp
    units = gate_matrix.shape[1] // n_fs
    padded = -(-units // 128) * 128
    slab = own_width // n_rep
    rep, fs, tp = lax.axis_index("rep"), lax.axis_index("fs"), lax.axis_index("tp")

    def slabs(matrix):
        rows = lax.dynamic_slice_in_dim(matrix, rep * slab, slab, axis=0).astype(half)
        rows = jnp.pad(rows.reshape(slab, n_fs, units), ((0, 0), (0, 0), (0, padded - units)))
        return jnp.transpose(rows, (1, 0, 2))

    weights = jnp.concatenate([slabs(m) for m in (gate_matrix, up_matrix, down_matrix)], axis=2)
    own_rows = residual.reshape(row_count, local_width)
    both_rows, both_scale = exchange(
        [own_rows, output_column_scale.reshape(1, local_width)], "tp", n_tp, False, 1
    )
    wide = jnp.transpose(both_rows, (1, 0, 2)).reshape(row_count, n_fs, n_tp, part)
    mine = lax.dynamic_index_in_dim(wide, tp, axis=2, keepdims=False)
    got_weights, got_rows = exchange(
        [weights, jnp.transpose(mine, (1, 0, 2))], "fs", n_fs, True, 2
    )
    all_weights = lax.all_gather(got_weights, "rep", axis=0, tiled=False)
    all_weights = jnp.transpose(all_weights, (1, 0, 2, 3)).reshape(width, 3 * padded)

    normalized_rows = linear_attend(
        queries, key_matrix, value_matrix, decay_logodds, decay_surge, head_norm_gain
    )
    gathered = gather(normalized_rows, n_fs, n_tp, False, 3)
    group_rows = n_fs * row_count
    mix_terms = by_rows(gathered.reshape(group_rows, -1), output_matrix.astype(half)).astype(half)
    mix_split = jnp.transpose(mix_terms.reshape(group_rows, n_tp, part), (1, 0, 2))
    (mix_parts,) = exchange([mix_split], "tp", n_tp, True, 4)
    mixed = jnp.sum(mix_parts.astype(jnp.float32), axis=0)
    out_scale = lax.dynamic_index_in_dim(
        lax.dynamic_index_in_dim(both_scale.reshape(n_fs, n_tp, part), fs, 0, False), tp, 0, False
    )
    piece = got_rows.reshape(group_rows, part).astype(jnp.float32) + out_scale * mixed
    everywhere = gather(piece.astype(half), n_fs, n_tp, True, 5)
    updated = jnp.transpose(everywhere, (2, 1, 0, 3)).reshape(group_rows, width)
    wide_rows = updated.astype(jnp.float32)
    factor = lax.rsqrt(jnp.mean(wide_rows * wide_rows, axis=-1, keepdims=True) + epsilon)
    normin = (wide_rows * factor * premix_norm_gain).astype(half)

    def unit_scale(scale):
        own = lax.dynamic_index_in_dim(scale.reshape(n_fs, units), fs, 0, False)
        return jnp.pad(own, (0, padded - units))

    both = jnp.dot(normin, all_weights[:, : 2 * padded], preferred_element_type=jnp.float32)
    gate_pre = both[:, :padded] * unit_scale(gate_column_scale)
    up_pre = both[:, padded:] * unit_scale(up_column_scale)
    hidden = (jax.nn.silu(gate_pre) * up_pre).astype(half)
    down_terms = jnp.concatenate(
        [
            by_rows(
                hidden, all_weights[t * local_width : (t + 1) * local_width, 2 * padded :]
            ).astype(half)[None]
            for t in range(n_tp)
        ],
        axis=0,
    )
    down_back = reduce_back(
        down_terms.reshape(n_tp, n_fs, row_count, local_width), n_fs, 7
    )
    down_total = jnp.sum(down_back.astype(jnp.float32), axis=0)
    own_updated = lax.dynamic_slice(
        updated, (fs * row_count, tp * local_width), (row_count, local_width)
    )
    result = (own_updated.astype(jnp.float32) + down_column_scale * down_total).astype(half)
    return result.reshape(sequence_batch, token_length, local_width)


def chosen_body(mesh):
    sizes = tuple(mesh.shape[name] for name in ("rep", "fs", "tp"))
    n_rep, n_fs, n_tp = sizes

    def run(*args):
        residual, output_matrix, gate_matrix = args[0], args[7], args[10]
        weights = output_matrix.size + 3 * gate_matrix.size
        rows = residual.shape[0] * residual.shape[1]
        moved = 3 * rows * residual.shape[2] + 3 * gate_matrix.size // n_rep
        fits = (
            n_fs == 4
            and n_tp == 2
            and output_matrix.shape[0] % (128 * n_tp) == 0
            and output_matrix.shape[0] % (16 * n_rep) == 0
        )
        if fits and moved < weights:
            return moving_body(sizes, *args)
        return body(*args)

    return run


def solution(mesh):
    return jax.shard_map(
        chosen_body(mesh),
        mesh=mesh,
        in_specs=(
            P(("rep", "fs"), None, "tp"),
            P(("rep", "fs"), None, "tp"),
            P(("rep", "fs"), None, "tp"),
            P(("rep", "fs"), None, "tp"),
            P(("rep", "fs"), None, "tp"),
            P(("rep", "fs"), None, "tp"),
            P(),
            P("fs", "tp"),
            P("tp"),
            P(),
            P("fs", "tp"),
            P("tp"),
            P("fs", "tp"),
            P("tp"),
            P("fs", "tp"),
            P("tp"),
        ),
        out_specs=P(("rep", "fs"), None, "tp"),
        check_vma=False,
    )
```

```python
import functools

import jax
import jax.numpy as jnp
from jax import lax
from jax.experimental import pallas as pl
from jax.experimental.pallas import tpu as pltpu
from jax.sharding import PartitionSpec as P

BLOCK = 64


epsilon = 1e-06
softness_factor = 16.0
highest = lax.Precision.HIGHEST


def attend_head(q, k, v, logodds, surge, gain):
    tokens, width = q.shape
    blocks = tokens // BLOCK
    mid = BLOCK // 2 - 1
    decay = (
        jnp.minimum(logodds, 0.0) - jnp.log1p(jnp.exp(-jnp.abs(logodds)))
    ) * (1.0 / softness_factor) + surge
    row = lax.broadcasted_iota(jnp.int32, (BLOCK, BLOCK), 0)
    col = lax.broadcasted_iota(jnp.int32, (BLOCK, BLOCK), 1)
    tri = jnp.where(row >= col, 1.0, 0.0).astype(jnp.bfloat16)
    q = q.astype(jnp.float32) * width ** (-0.5)
    k = k.astype(jnp.float32)
    high = decay.astype(jnp.bfloat16)
    low = (decay - high.astype(jnp.float32)).astype(jnp.bfloat16)
    pieces = []
    for n in range(blocks):
        rows = slice(n * BLOCK, (n + 1) * BLOCK)
        running = jnp.dot(tri, high[rows], preferred_element_type=jnp.float32) + jnp.dot(
            tri, low[rows], preferred_element_type=jnp.float32
        )
        before = running - decay[rows]
        center = running[mid : mid + 1]
        end = running[BLOCK - 1 : BLOCK]
        to_center = jnp.exp(center)
        from_center = jnp.exp(end - center)
        q_forward = q[rows] * jnp.exp(running - center)
        k_forward = k[rows] * jnp.exp(center - running)
        q_backward = q[rows] * jnp.exp(center - before)
        k_backward = k[rows] * jnp.exp(before - center)
        half = jnp.bfloat16
        scores = jnp.where(
            row >= col, by_rows(q_forward.astype(half), k_forward.astype(half)), 0.0
        ) + jnp.where(row <= col, by_rows(q_backward.astype(half), k_backward.astype(half)), 0.0)
        inner = jnp.dot(scores.astype(half), v[rows], preferred_element_type=jnp.float32)
        pieces.append(
            (
                inner,
                (q_forward * to_center).astype(half),
                (q_backward * from_center).astype(half),
                by_columns(v[rows], (k_forward * from_center).astype(half)),
                by_columns(v[rows], (k_backward * to_center).astype(half)),
                jnp.exp(end),
            )
        )
    totals = [piece[0] for piece in pieces]
    state = None
    for n in range(blocks):
        if state is not None:
            totals[n] = totals[n] + by_rows(pieces[n][1], state.astype(jnp.bfloat16))
        state = pieces[n][3] if state is None else pieces[n][5] * state + pieces[n][3]
    state = None
    for n in reversed(range(blocks)):
        if state is not None:
            totals[n] = totals[n] + by_rows(pieces[n][2], state.astype(jnp.bfloat16))
        state = pieces[n][4] if state is None else pieces[n][5] * state + pieces[n][4]
    attended = jnp.concatenate(totals, axis=0)
    scale = lax.rsqrt(jnp.mean(attended * attended, axis=-1, keepdims=True) + epsilon)
    return (attended * scale * gain).astype(jnp.bfloat16)


def by_columns(left, right):
    return lax.dot_general(
        left, right, (((0,), (0,)), ((), ())), preferred_element_type=jnp.float32
    )


def attend_kernel(head_total, q_ref, k_ref, v_ref, lo_ref, sg_ref, gain_ref, out_ref):
    width = q_ref.shape[1] // head_total
    value_width = v_ref.shape[1] // head_total
    for h in range(head_total):
        keys = slice(h * width, (h + 1) * width)
        values = slice(h * value_width, (h + 1) * value_width)
        out_ref[:, values] = attend_head(
            q_ref[:, keys],
            k_ref[:, keys],
            v_ref[:, values],
            lo_ref[:, keys],
            sg_ref[:, h : h + 1],
            gain_ref[...],
        )


def linear_attend(queries, key_matrix, value_matrix, decay_logodds, decay_surge, head_norm_gain):
    _, token_length, head_total = decay_surge.shape
    outs = [
        pl.pallas_call(
            functools.partial(attend_kernel, head_total),
            out_shape=jax.ShapeDtypeStruct(value_matrix.shape[1:], jnp.bfloat16),
            in_specs=[pl.BlockSpec(memory_space=pltpu.VMEM)] * 6,
            out_specs=pl.BlockSpec(memory_space=pltpu.VMEM),
            cost_estimate=pl.CostEstimate(
                flops=10**9, bytes_accessed=4 * 10**6, transcendentals=10**6
            ),
        )(
            queries[b], key_matrix[b], value_matrix[b], decay_logodds[b], decay_surge[b],
            head_norm_gain.reshape(1, -1),
        )
        for b in range(queries.shape[0])
    ]
    return jnp.concatenate(outs, axis=0)


def by_rows(left, right):
    return lax.dot_general(
        left, right, (((1,), (1,)), ((), ())), preferred_element_type=jnp.float32
    )


def body(
    residual,
    queries,
    key_matrix,
    value_matrix,
    decay_logodds,
    decay_surge,
    head_norm_gain,
    output_matrix,
    output_column_scale,
    premix_norm_gain,
    gate_matrix,
    gate_column_scale,
    up_matrix,
    up_column_scale,
    down_matrix,
    down_column_scale,
):
    sequence_batch, token_length, local_width = residual.shape
    row_count = sequence_batch * token_length
    normalized_rows = linear_attend(
        queries, key_matrix, value_matrix, decay_logodds, decay_surge, head_norm_gain
    )
    out_half = output_matrix.astype(jnp.bfloat16)
    out_full = lax.all_gather(out_half, "fs", axis=0, tiled=True)
    mix_terms = by_rows(normalized_rows, out_full)
    mix_total = lax.psum_scatter(
        mix_terms.astype(jnp.bfloat16), "tp", scatter_dimension=1, tiled=True
    ).astype(jnp.float32)
    own_rows = residual.reshape(row_count, local_width).astype(jnp.float32)
    updated = (own_rows + output_column_scale * mix_total).astype(jnp.bfloat16)
    features = lax.all_gather(updated, "tp", axis=1, tiled=True)
    wide_rows = features.astype(jnp.float32)
    factor = lax.rsqrt(jnp.mean(wide_rows * wide_rows, axis=-1, keepdims=True) + epsilon)
    normin = (wide_rows * factor * premix_norm_gain).astype(jnp.bfloat16)
    gate_half = gate_matrix.astype(jnp.bfloat16)
    up_half = up_matrix.astype(jnp.bfloat16)
    down_half = down_matrix.astype(jnp.bfloat16)
    gate_full, up_full, down_full = (
        lax.all_gather(gate_half, "fs", axis=0, tiled=True),
        lax.all_gather(up_half, "fs", axis=0, tiled=True),
        lax.all_gather(down_half, "fs", axis=0, tiled=True),
    )
    gate_pre = jnp.dot(normin, gate_full, preferred_element_type=jnp.float32)
    up_pre = jnp.dot(normin, up_full, preferred_element_type=jnp.float32)
    hidden = (jax.nn.silu(gate_pre * gate_column_scale) * (up_pre * up_column_scale)).astype(
        jnp.bfloat16
    )
    down_terms = by_rows(hidden, down_full)
    down_total = lax.psum_scatter(
        down_terms.astype(jnp.bfloat16), "tp", scatter_dimension=1, tiled=True
    ).astype(jnp.float32)
    result = (updated.astype(jnp.float32) + down_column_scale * down_total).astype(jnp.bfloat16)
    return result.reshape(sequence_batch, token_length, local_width)


def exchange_kernel(axis, n, spread, count, *refs):
    ins, outs = refs[:count], refs[count : 2 * count]
    send_sem, recv_sem = refs[2 * count :]
    me = lax.axis_index(axis)
    barrier = pltpu.get_barrier_semaphore()
    for step in range(1, n):
        pl.semaphore_signal(
            barrier,
            inc=1,
            device_id={axis: lax.rem(me + step, n)},
            device_id_type=pl.DeviceIdType.MESH,
        )
    pl.semaphore_wait(barrier, n - 1)
    copies = []
    for step in range(1, n):
        peer = lax.rem(me + step, n)
        for c in range(count):
            copy = pltpu.make_async_remote_copy(
                src_ref=ins[c].at[peer] if spread else ins[c],
                dst_ref=outs[c].at[me],
                send_sem=send_sem.at[c, step - 1],
                recv_sem=recv_sem.at[c, step - 1],
                device_id={axis: peer},
                device_id_type=pl.DeviceIdType.MESH,
            )
            copy.start()
            copies.append(copy)
    for c in range(count):
        outs[c][me] = ins[c][me] if spread else ins[c][...]
    for copy in copies:
        copy.wait()


def exchange(arrays, axis, n, spread, call):
    count = len(arrays)
    shapes = [a.shape if spread else (n,) + a.shape for a in arrays]
    return pl.pallas_call(
        functools.partial(exchange_kernel, axis, n, spread, count),
        out_shape=[jax.ShapeDtypeStruct(d, a.dtype) for d, a in zip(shapes, arrays)],
        in_specs=[pl.BlockSpec(memory_space=pltpu.VMEM)] * count,
        out_specs=[pl.BlockSpec(memory_space=pltpu.VMEM)] * count,
        scratch_shapes=[
            pltpu.SemaphoreType.DMA((count, n - 1)),
            pltpu.SemaphoreType.DMA((count, n - 1)),
        ],
        compiler_params=pltpu.CompilerParams(collective_id=call, has_side_effects=True),
        cost_estimate=pl.CostEstimate(
            flops=10**9, bytes_accessed=2 * 10**7, transcendentals=0
        ),
    )(*arrays)


def send(source, target, sems, index, device):
    copy = pltpu.make_async_remote_copy(
        src_ref=source,
        dst_ref=target,
        send_sem=sems[0].at[index],
        recv_sem=sems[1].at[index],
        device_id=device,
        device_id_type=pl.DeviceIdType.MESH,
    )
    copy.start()
    return copy


def greet(devices):
    barrier = pltpu.get_barrier_semaphore()
    for device in devices:
        pl.semaphore_signal(
            barrier, inc=1, device_id=device, device_id_type=pl.DeviceIdType.MESH
        )
    pl.semaphore_wait(barrier, len(devices))


def gather_kernel(share, x_ref, out_ref, *sems):
    me, tp = lax.axis_index("fs"), lax.axis_index("tp")
    near = me + 1 - 2 * lax.rem(me, 2)
    far = lax.rem(me + 2, 4)
    corner = lax.rem(near + 2, 4)
    to_near, to_far, to_pair = {"fs": near}, {"fs": far}, {"tp": 1 - tp}
    greet([to_near, to_far] + ([to_pair] if share else []))
    own = out_ref.at[tp] if share else out_ref
    rows = x_ref.shape[0] // 2
    upper, lower = pl.ds(0, rows), pl.ds(rows, rows)
    near_upper = send(x_ref.at[upper], own.at[me, upper], sems, 0, to_near)
    far_lower = send(x_ref.at[lower], own.at[me, lower], sems, 1, to_far)
    near_lower = send(x_ref.at[lower], own.at[me, lower], sems, 2, to_near)
    far_upper = send(x_ref.at[upper], own.at[me, upper], sems, 3, to_far)
    copies = [near_upper, far_lower, near_lower, far_upper]
    shared = [send(x_ref, own.at[me], sems, 6, to_pair)] if share else []
    own[me] = x_ref[...]
    near_upper.wait_recv()
    corner_upper = send(own.at[near, upper], own.at[near, upper], sems, 4, to_far)
    far_lower.wait_recv()
    corner_lower = send(own.at[far, lower], own.at[far, lower], sems, 5, to_near)
    near_lower.wait_recv()
    if share:
        shared.append(send(own.at[near], own.at[near], sems, 7, to_pair))
    far_upper.wait_recv()
    if share:
        shared.append(send(own.at[far], own.at[far], sems, 8, to_pair))
    corner_upper.wait_recv()
    corner_lower.wait_recv()
    if share:
        shared.append(send(own.at[corner], own.at[corner], sems, 9, to_pair))
    for copy in copies + [corner_upper, corner_lower]:
        copy.wait_send()
    for copy in shared:
        copy.wait()


def gather(x, n_fs, n_tp, share, call):
    shape = ((n_tp,) if share else ()) + (n_fs,) + x.shape
    return pl.pallas_call(
        functools.partial(gather_kernel, share),
        out_shape=jax.ShapeDtypeStruct(shape, x.dtype),
        in_specs=[pl.BlockSpec(memory_space=pltpu.VMEM)],
        out_specs=pl.BlockSpec(memory_space=pltpu.VMEM),
        scratch_shapes=[pltpu.SemaphoreType.DMA((10,)), pltpu.SemaphoreType.DMA((10,))],
        compiler_params=pltpu.CompilerParams(collective_id=call, has_side_effects=True),
        cost_estimate=pl.CostEstimate(
            flops=10**9, bytes_accessed=2 * 10**7, transcendentals=0
        ),
    )(x)


def reduce_kernel(n, terms_ref, back_ref, part_ref, total_ref, *sems):
    me, tp = lax.axis_index("fs"), lax.axis_index("tp")
    steps = list(range(1, n)) + [0]
    peers = [lax.rem(me + step, n) for step in range(n)]
    greet([{"fs": peers[step]} for step in range(1, n)] + [{"tp": 1 - tp}])
    pairs = {
        step: send(
            terms_ref.at[1 - tp, peers[step]], part_ref.at[peers[step]], sems, step, {"tp": 1 - tp}
        )
        for step in steps
    }
    copies = []
    for step in steps:
        peer = peers[step]
        pairs[step].wait_recv()
        total = terms_ref[tp, peer].astype(jnp.float32) + part_ref[peer].astype(jnp.float32)
        if step == 0:
            back_ref[me] = total.astype(back_ref.dtype)
        else:
            total_ref[peer] = total.astype(back_ref.dtype)
            copies.append(
                send(total_ref.at[peer], back_ref.at[me], sems, n + step, {"fs": peer})
            )
    for step in steps:
        pairs[step].wait_send()
    for copy in copies:
        copy.wait()


def reduce_back(terms, n_fs, call):
    shape = terms.shape[1:]
    return pl.pallas_call(
        functools.partial(reduce_kernel, n_fs),
        out_shape=jax.ShapeDtypeStruct(shape, terms.dtype),
        in_specs=[pl.BlockSpec(memory_space=pltpu.VMEM)],
        out_specs=pl.BlockSpec(memory_space=pltpu.VMEM),
        scratch_shapes=[
            pltpu.VMEM(shape, terms.dtype),
            pltpu.VMEM(shape, terms.dtype),
            pltpu.SemaphoreType.DMA((2 * n_fs,)),
            pltpu.SemaphoreType.DMA((2 * n_fs,)),
        ],
        compiler_params=pltpu.CompilerParams(collective_id=call, has_side_effects=True),
        cost_estimate=pl.CostEstimate(
            flops=10**9, bytes_accessed=2 * 10**7, transcendentals=0
        ),
    )(terms)


def pack_kernel(n, units, padded, *refs):
    matrices, out_ref, held, sems = refs[:3], refs[3], refs[4], refs[5]
    slab = held.shape[1]
    rows = pl.ds(pl.multiple_of(lax.axis_index("rep") * slab, slab), slab)
    copies = [
        pltpu.make_async_copy(matrix.at[rows], held.at[m], sems.at[m])
        for m, matrix in enumerate(matrices)
    ]
    for copy in copies:
        copy.start()
    for m, copy in enumerate(copies):
        copy.wait()
        for j in range(n):
            own = held[m, :, j * units : (j + 1) * units]
            if padded > units:
                fill = jnp.zeros((slab, padded - units), own.dtype)
                own = jnp.concatenate([own, fill], axis=1)
            out_ref[j, :, m * padded : (m + 1) * padded] = own.astype(out_ref.dtype)


def pack(matrices, n, units, padded, slab):
    return pl.pallas_call(
        functools.partial(pack_kernel, n, units, padded),
        out_shape=jax.ShapeDtypeStruct((n, slab, 3 * padded), jnp.bfloat16),
        in_specs=[pl.BlockSpec(memory_space=pl.ANY)] * 3,
        out_specs=pl.BlockSpec(memory_space=pltpu.VMEM),
        scratch_shapes=[
            pltpu.VMEM((3, slab, matrices[0].shape[1]), jnp.float32),
            pltpu.SemaphoreType.DMA((3,)),
        ],
        cost_estimate=pl.CostEstimate(
            flops=10**6, bytes_accessed=4 * 10**6, transcendentals=0
        ),
    )(*matrices)


def moving_body(
    sizes,
    residual,
    queries,
    key_matrix,
    value_matrix,
    decay_logodds,
    decay_surge,
    head_norm_gain,
    output_matrix,
    output_column_scale,
    premix_norm_gain,
    gate_matrix,
    gate_column_scale,
    up_matrix,
    up_column_scale,
    down_matrix,
    down_column_scale,
):
    n_rep, n_fs, n_tp = sizes
    half = jnp.bfloat16
    sequence_batch, token_length, local_width = residual.shape
    row_count = sequence_batch * token_length
    width = local_width * n_tp
    own_width = output_matrix.shape[0]
    part = own_width // n_tp
    units = gate_matrix.shape[1] // n_fs
    padded = -(-units // 128) * 128
    slab = own_width // n_rep
    rep, fs, tp = lax.axis_index("rep"), lax.axis_index("fs"), lax.axis_index("tp")

    weights = pack((gate_matrix, up_matrix, down_matrix), n_fs, units, padded, slab)
    own_rows = residual.reshape(row_count, local_width)
    both_rows, both_scale = exchange(
        [own_rows, output_column_scale.reshape(1, local_width)], "tp", n_tp, False, 1
    )
    wide = jnp.transpose(both_rows, (1, 0, 2)).reshape(row_count, n_fs, n_tp, part)
    mine = lax.dynamic_index_in_dim(wide, tp, axis=2, keepdims=False)
    got_weights, got_rows = exchange(
        [weights, jnp.transpose(mine, (1, 0, 2))], "fs", n_fs, True, 2
    )
    all_weights = lax.all_gather(got_weights, "rep", axis=0, tiled=False)
    all_weights = jnp.transpose(all_weights, (1, 0, 2, 3)).reshape(width, 3 * padded)

    normalized_rows = linear_attend(
        queries, key_matrix, value_matrix, decay_logodds, decay_surge, head_norm_gain
    )
    gathered = gather(normalized_rows, n_fs, n_tp, False, 3)
    group_rows = n_fs * row_count
    mix_terms = by_rows(gathered.reshape(group_rows, -1), output_matrix.astype(half)).astype(half)
    mix_split = jnp.transpose(mix_terms.reshape(group_rows, n_tp, part), (1, 0, 2))
    (mix_parts,) = exchange([mix_split], "tp", n_tp, True, 4)
    mixed = jnp.sum(mix_parts.astype(jnp.float32), axis=0)
    out_scale = lax.dynamic_index_in_dim(
        lax.dynamic_index_in_dim(both_scale.reshape(n_fs, n_tp, part), fs, 0, False), tp, 0, False
    )
    piece = got_rows.reshape(group_rows, part).astype(jnp.float32) + out_scale * mixed
    everywhere = gather(piece.astype(half), n_fs, n_tp, True, 5)
    updated = jnp.transpose(everywhere, (2, 1, 0, 3)).reshape(group_rows, width)
    wide_rows = updated.astype(jnp.float32)
    factor = lax.rsqrt(jnp.mean(wide_rows * wide_rows, axis=-1, keepdims=True) + epsilon)
    normin = (wide_rows * factor * premix_norm_gain).astype(half)

    def unit_scale(scale):
        own = lax.dynamic_index_in_dim(scale.reshape(n_fs, units), fs, 0, False)
        return jnp.pad(own, (0, padded - units))

    both = jnp.dot(normin, all_weights[:, : 2 * padded], preferred_element_type=jnp.float32)
    gate_pre = both[:, :padded] * unit_scale(gate_column_scale)
    up_pre = both[:, padded:] * unit_scale(up_column_scale)
    hidden = (jax.nn.silu(gate_pre) * up_pre).astype(half)
    down_terms = jnp.concatenate(
        [
            by_rows(
                hidden, all_weights[t * local_width : (t + 1) * local_width, 2 * padded :]
            ).astype(half)[None]
            for t in range(n_tp)
        ],
        axis=0,
    )
    down_back = reduce_back(
        down_terms.reshape(n_tp, n_fs, row_count, local_width), n_fs, 7
    )
    down_total = jnp.sum(down_back.astype(jnp.float32), axis=0)
    own_updated = lax.dynamic_slice(
        updated, (fs * row_count, tp * local_width), (row_count, local_width)
    )
    result = (own_updated.astype(jnp.float32) + down_column_scale * down_total).astype(half)
    return result.reshape(sequence_batch, token_length, local_width)


def chosen_body(mesh):
    sizes = tuple(mesh.shape[name] for name in ("rep", "fs", "tp"))
    n_rep, n_fs, n_tp = sizes

    def run(*args):
        residual, output_matrix, gate_matrix = args[0], args[7], args[10]
        weights = output_matrix.size + 3 * gate_matrix.size
        rows = residual.shape[0] * residual.shape[1]
        moved = 3 * rows * residual.shape[2] + 3 * gate_matrix.size // n_rep
        fits = (
            n_fs == 4
            and n_tp == 2
            and output_matrix.shape[0] % (128 * n_tp) == 0
            and output_matrix.shape[0] % (16 * n_rep) == 0
        )
        if fits and moved < weights:
            return moving_body(sizes, *args)
        return body(*args)

    return run


def solution(mesh):
    return jax.shard_map(
        chosen_body(mesh),
        mesh=mesh,
        in_specs=(
            P(("rep", "fs"), None, "tp"),
            P(("rep", "fs"), None, "tp"),
            P(("rep", "fs"), None, "tp"),
            P(("rep", "fs"), None, "tp"),
            P(("rep", "fs"), None, "tp"),
            P(("rep", "fs"), None, "tp"),
            P(),
            P("fs", "tp"),
            P("tp"),
            P(),
            P("fs", "tp"),
            P("tp"),
            P("fs", "tp"),
            P("tp"),
            P("fs", "tp"),
            P("tp"),
        ),
        out_specs=P(("rep", "fs"), None, "tp"),
        check_vma=False,
    )
```
